32 devices in a mesh: sp: 8 (over z, x), tp: 4 (over y, core).
Axes of the slice: x: 2, y: 2, z: 4, core: 2. Of those that a mesh axis runs over, the one named last changes fastest.
Arguments:
- tokens: bfloat16 [8192, 2048], P('sp', 'tp'), may hold values from -6 to 6
- norm_gain: float32 [2048], replicated, may hold values from 0.1 to 1.9
- att_query: bfloat16 [2048, 1024], P(None, 'tp'), may hold values from -1 to 1, as said below
- att_key: bfloat16 [2048, 512], P(None, 'tp'), may hold values from -16 to 16, as said below
- att_value: bfloat16 [2048, 512], P(None, 'tp'), may hold values from -0.125 to 0.125
- ret_query: bfloat16 [2048, 512], P(None, 'tp'), may hold values from -0.125 to 0.125
- ret_key: bfloat16 [2048, 512], P(None, 'tp'), may hold values from -0.125 to 0.125
- ret_value: bfloat16 [2048, 1024], P(None, 'tp'), may hold values from -0.125 to 0.125
- ret_gate: bfloat16 [2048, 1024], P(None, 'tp'), may hold values from -0.125 to 0.125
- att_sink: float32 [16], P('tp'), may hold values from 4 to 7
- decay_log: float32 [8, 8192], P('tp', 'sp'), may hold values from -2 to 0, as said below
- init_state: float32 [2, 8, 64, 128], P(None, 'tp'), may hold values from -24 to 24
- out_att: bfloat16 [1024, 2048], P('tp'), may hold values from -0.125 to 0.125
- out_ret: bfloat16 [1024, 2048], P('tp'), may hold values from -0.125 to 0.125
Outputs:
- mixed: bfloat16 [8192, 2048], P('sp', 'tp')
The draws below stay inside these ranges and needn't reach their ends.
Inputs may be any that keep to these rules, and one draw needn't show every extreme that they name: `att_query`: entries of order D ** -0.5. `att_key`: entries of order D ** -0.5 or larger. `decay_log`: log decays, negative.
All inputs are finite; a program needn't handle non-finite values.
Results may differ from the reference program's by a relative error of at most 0.02.
Values may be sent and summed in bfloat16 or wider, within the bound.
A program may use at most 64 MiB of HBM per device.

```python
import math
import jax
import jax.numpy as jnp
from jax import lax

D = 2048
ATT_HEADS = 16
KV_HEADS = 8
HD = 64
RET_HEADS = 8
RK = 64
RV = 128
WINDOW = 128
RET_BLOCK = 128
TOK_DEV = 1024
SEQUENCE_LENGTH = 8192
N_TP = 4


def draw_tokens(key, part):
    base_rows = jnp.clip(jax.random.normal(key, (SEQUENCE_LENGTH, D), jnp.float32), -6.0, 6.0)
    return base_rows.astype(jnp.bfloat16)


def attention_weights(key):
    query_w = jnp.clip(jax.random.normal(jax.random.fold_in(key, 11), (D, ATT_HEADS * HD), jnp.float32), -4.0, 4.0) * D ** (-0.5)
    key_w = jnp.clip(jax.random.normal(jax.random.fold_in(key, 12), (D, KV_HEADS * HD), jnp.float32), -4.0, 4.0) * D ** (-0.5)
    return (query_w, key_w)


def draw_att_query(key, part):
    return attention_weights(key)[0].astype(jnp.bfloat16)


def draw_att_key(key, part):
    return attention_weights(key)[1].astype(jnp.bfloat16)


def draw_decay_log(key, part):
    child_random_keys = jax.random.split(key, 7)
    slow_heads = jax.random.uniform(child_random_keys[0], (RET_HEADS,)) < 0.5
    slow_rate = 0.15 * math.log(10.0) / SEQUENCE_LENGTH * jax.random.uniform(child_random_keys[1], (RET_HEADS,), minval=0.5, maxval=1.5)
    fast_rate = jax.random.uniform(child_random_keys[2], (RET_HEADS,), minval=1.0 / 100.0, maxval=1.0 / 30.0)
    baseline_rate = jnp.where(slow_heads, slow_rate, fast_rate)
    device_pace = jnp.exp(jax.random.uniform(child_random_keys[3], (SEQUENCE_LENGTH // TOK_DEV,), minval=math.log(0.5), maxval=math.log(2.0)))
    full_speed = jnp.repeat(device_pace, TOK_DEV, total_repeat_length=SEQUENCE_LENGTH)
    jaggedness = jax.random.uniform(child_random_keys[4], (RET_HEADS, SEQUENCE_LENGTH), minval=0.5, maxval=1.5)
    spike_positions = jax.random.randint(child_random_keys[5], (3,), 0, SEQUENCE_LENGTH)
    spike_depth = jax.random.uniform(child_random_keys[6], (3,), minval=0.55, maxval=0.85)
    spike_count = jnp.zeros((SEQUENCE_LENGTH,), jnp.float32).at[spike_positions].add(jnp.log(spike_depth))
    return -baseline_rate[:, None] * full_speed[None, :] * jaggedness + spike_count[None, :]


def block_scale(rng, dims, pieces, smallest, largest):
    def one(position, shards_of):
        heights = jax.random.uniform(jax.random.fold_in(jax.random.fold_in(rng, 6), position), (shards_of,), jnp.float32, smallest / len(pieces), largest / len(pieces))
        return jnp.repeat(jnp.exp(heights), dims[position] // shards_of).reshape((-1,) + (1,) * (len(dims) - position - 1))

    loudness = one(*pieces[0])
    for cut in pieces[1:]:
        loudness = loudness * one(*cut)
    return loudness


def scatter_about(own_key, extent, scale, limit, cuts=(), held_as=jnp.bfloat16):
    result = jax.random.normal(own_key, extent, jnp.float32) * scale
    if len(cuts) > 0:
        result = block_scale(own_key, extent, cuts, -0.22, 0.18) * result
    return jnp.clip(result, min=-limit, max=limit).astype(held_as)


def setup_inputs(seed: int = 0) -> dict:
    seeds = jax.random.split(jax.random.key(seed), 15)
    tokens = draw_tokens(jax.random.fold_in(seeds[14], 71), 0)
    norm_gain = jnp.clip(1.0 + 0.18 * jax.random.normal(seeds[1], (D,), jnp.float32), 0.1, 1.9)
    att_query = draw_att_query(jax.random.fold_in(seeds[14], 71), 0)
    att_key = draw_att_key(jax.random.fold_in(seeds[14], 71), 0)
    att_value = scatter_about(seeds[4], (D, KV_HEADS * HD), D ** -0.5, 0.125, ((1, 4),))
    ret_query = scatter_about(seeds[5], (D, RET_HEADS * RK), D ** -0.5, 0.125, ((1, 4),))
    ret_key = scatter_about(seeds[6], (D, RET_HEADS * RK), D ** -0.5, 0.125, ((1, 4),))
    ret_value = scatter_about(seeds[7], (D, RET_HEADS * RV), D ** -0.5, 0.125, ((1, 4),))
    ret_gate = scatter_about(seeds[8], (D, RET_HEADS * RV), D ** -0.5, 0.125, ((1, 4),))
    att_sink = jnp.clip(4.0 + 3.0 * jax.random.uniform(seeds[9], (ATT_HEADS,), jnp.float32) ** block_scale(seeds[9], (ATT_HEADS,), ((0, 4),), -0.2, 0.2), 4.0, 7.0)
    decay_log = draw_decay_log(jax.random.fold_in(seeds[14], 71), 0)
    init_state = scatter_about(seeds[11], (2, RET_HEADS, RK, RV), 4.0, 24.0, ((1, 4),), jnp.float32)
    out_att = scatter_about(seeds[12], (ATT_HEADS * HD, D), (ATT_HEADS * HD + RET_HEADS * RV) ** -0.5, 0.125, ((0, 4),))
    out_ret = scatter_about(seeds[13], (RET_HEADS * RV, D), (ATT_HEADS * HD + RET_HEADS * RV) ** -0.5, 0.125, ((0, 4),))
    return dict(tokens=tokens, norm_gain=norm_gain, att_query=att_query, att_key=att_key, att_value=att_value, ret_query=ret_query, ret_key=ret_key, ret_value=ret_value, ret_gate=ret_gate, att_sink=att_sink, decay_log=decay_log, init_state=init_state, out_att=out_att, out_ret=out_ret)


NORM_EPS = 1e-06
ROPE_BASE = 10000.0
HIGHEST = lax.Precision.HIGHEST

def rotated(values, positions):
    half_dim = values.shape[-1] // 2
    inverse = ROPE_BASE ** (-2.0 * jnp.arange(half_dim, dtype=jnp.float32) / values.shape[-1])
    angles = positions.astype(jnp.float32)[:, None] * inverse[None, :]
    cosine = jnp.cos(angles)[:, None, :]
    sine = jnp.sin(angles)[:, None, :]
    first_half = values[..., :half_dim]
    second_half = values[..., half_dim:]
    return jnp.concatenate([first_half * cosine - second_half * sine, first_half * sine + second_half * cosine], axis=-1)

def attend_all(queries, key_proj, value_proj, att_sink):
    seq_len = queries.shape[0]
    block_rows = 512
    groups = ATT_HEADS // KV_HEADS
    span_rows = block_rows + 2 * WINDOW
    padded_keys = jnp.pad(key_proj, ((WINDOW, WINDOW), (0, 0)))
    padded_vals = jnp.pad(value_proj, ((WINDOW, WINDOW), (0, 0)))
    sink_col = att_sink.astype(jnp.float32).reshape(KV_HEADS, groups, 1, 1)

    def one_block(block_index):
        first_row = block_index * block_rows
        query_block = lax.dynamic_slice_in_dim(queries, first_row, block_rows, 0).reshape(block_rows, KV_HEADS, groups, HD)
        key_block = lax.dynamic_slice_in_dim(padded_keys, first_row, span_rows, 0).reshape(span_rows, KV_HEADS, HD)
        value_block = lax.dynamic_slice_in_dim(padded_vals, first_row, span_rows, 0).reshape(span_rows, KV_HEADS, HD)
        scores = jnp.einsum('qkgd,skd->kgqs', query_block.astype(jnp.float32), key_block.astype(jnp.float32)) * HD ** (-0.5)
        query_pos = first_row + jnp.arange(block_rows, dtype=jnp.int32)
        key_pos = first_row - WINDOW + jnp.arange(span_rows, dtype=jnp.int32)
        allowed = (jnp.abs(query_pos[:, None] - key_pos[None, :]) <= WINDOW) & (key_pos >= 0)[None, :] & (key_pos < seq_len)[None, :]
        scores = jnp.where(allowed, scores, -jnp.inf)
        row_top = jnp.maximum(lax.optimization_barrier(jnp.max(scores, axis=-1, keepdims=True)), sink_col)
        raised = jnp.exp(scores - row_top)
        denominator = lax.optimization_barrier(jnp.sum(raised, axis=-1, keepdims=True)) + jnp.exp(sink_col - row_top)
        weights_bf = (raised / denominator).astype(jnp.bfloat16)
        block_out = jnp.einsum('kgqs,skd->qkgd', weights_bf.astype(jnp.float32), value_block.astype(jnp.float32))
        return block_out.reshape(block_rows, ATT_HEADS * HD).astype(jnp.bfloat16)
    blocks = lax.map(one_block, jnp.arange(seq_len // block_rows, dtype=jnp.int32))
    return blocks.reshape(seq_len, ATT_HEADS * HD)

def advance(state_now, item_pair):
    factor_now, term_now = item_pair
    return (factor_now[:, None, None] * state_now + term_now, state_now)

def retain_all(query_rot, key_rot, value_f, decay_log, init_state):
    seq_len = query_rot.shape[0]
    block_count = seq_len // RET_BLOCK

    def heads_first(values, width):
        return jnp.transpose(values.reshape(block_count, RET_BLOCK, RET_HEADS, width), (2, 0, 1, 3))
    query_h = heads_first(query_rot, RK)
    key_h = heads_first(key_rot, RK)
    value_h = heads_first(value_f, RV)
    block_logs = decay_log.reshape(RET_HEADS, block_count, RET_BLOCK)
    cumul = jnp.cumsum(block_logs, axis=-1)
    block_log = cumul[..., -1]
    inner_w = jnp.einsum('hbnk,hbmk->hbnm', query_h, key_h, precision=HIGHEST) * jnp.exp(-jnp.abs(cumul[..., :, None] - cumul[..., None, :]))
    local_out = jnp.einsum('hbnm,hbmv->hbnv', inner_w, value_h, precision=HIGHEST)
    fwd_terms = jnp.einsum('hbmk,hbmv->bhkv', key_h * jnp.exp(block_log[..., None] - cumul)[..., None], value_h, precision=HIGHEST)
    bwd_terms = jnp.einsum('hbmk,hbmv->bhkv', key_h * jnp.exp(cumul)[..., None], value_h, precision=HIGHEST)
    factors = jnp.exp(block_log).T
    _, fwd_in = lax.scan(advance, init_state[0], (factors, fwd_terms))
    _, bwd_in = lax.scan(advance, init_state[1], (factors, bwd_terms), reverse=True)
    cross_out = jnp.exp(cumul)[..., None] * jnp.einsum('hbnk,bhkv->hbnv', query_h, fwd_in, precision=HIGHEST)
    cross_out = cross_out + jnp.exp(block_log[..., None] - cumul)[..., None] * jnp.einsum('hbnk,bhkv->hbnv', query_h, bwd_in, precision=HIGHEST)
    combined = local_out + cross_out
    centered = combined - lax.optimization_barrier(jnp.mean(combined, axis=-1, keepdims=True))
    normed = centered * lax.rsqrt(lax.optimization_barrier(jnp.mean(centered * centered, axis=-1, keepdims=True)) + NORM_EPS)
    return jnp.transpose(normed, (1, 2, 0, 3)).reshape(seq_len, RET_HEADS * RV)

def reference(tokens, norm_gain, att_query, att_key, att_value, ret_query, ret_key, ret_value, ret_gate, att_sink, decay_log, init_state, out_att, out_ret):
    seq_len = tokens.shape[0]
    tokens_f = tokens.astype(jnp.float32)
    inv_rms = lax.rsqrt(lax.optimization_barrier(jnp.mean(tokens_f * tokens_f, axis=-1, keepdims=True)) + NORM_EPS)
    normed = (tokens_f * norm_gain.astype(jnp.float32)[None, :]).astype(jnp.bfloat16)

    def project(weight):
        return (jnp.dot(normed, weight, preferred_element_type=jnp.float32) * inv_rms).astype(jnp.bfloat16)
    attended = attend_all(project(att_query), project(att_key), project(att_value), att_sink)
    positions = jnp.arange(seq_len, dtype=jnp.int32)
    query_rot = rotated(project(ret_query).astype(jnp.float32).reshape(seq_len, RET_HEADS, RK), positions)
    key_rot = rotated(project(ret_key).astype(jnp.float32).reshape(seq_len, RET_HEADS, RK), positions) * RK ** (-0.5)
    value_f = project(ret_value).astype(jnp.float32).reshape(seq_len, RET_HEADS, RV)
    retained = retain_all(query_rot, key_rot, value_f, decay_log, init_state)
    gate_f = project(ret_gate).astype(jnp.float32)
    ret_out = (jax.nn.silu(gate_f) * retained).astype(jnp.bfloat16)
    att_width = ATT_HEADS * HD // N_TP
    ret_width = RET_HEADS * RV // N_TP
    summed = jnp.zeros((seq_len, D), jnp.float32)
    for group_index in range(N_TP):
        att_lo = group_index * att_width
        ret_lo = group_index * ret_width
        partial_sum = jnp.dot(attended[:, att_lo:att_lo + att_width], out_att[att_lo:att_lo + att_width], preferred_element_type=jnp.float32)
        partial_sum = partial_sum + jnp.dot(ret_out[:, ret_lo:ret_lo + ret_width], out_ret[ret_lo:ret_lo + ret_width], preferred_element_type=jnp.float32)
        rounded = lax.optimization_barrier(partial_sum.astype(jnp.bfloat16))
        summed = summed + rounded.astype(jnp.float32)
    return summed.astype(jnp.bfloat16)
```

```python
import jax
import jax.numpy as jnp
from jax import lax
from jax.sharding import PartitionSpec as P

HD = 64
RK = 64
RV = 128
WINDOW = 128
RET_BLOCK = 128


NORM_EPS = 1e-06
ROPE_BASE = 10000.0
HIGHEST = lax.Precision.HIGHEST


def padded_2(block, sides, width):
    for axis, dim in sides:
        count = lax.axis_size(axis)
        forward = [(i, i + 1) for i in range(count - 1)]
        backward = [(target, source) for source, target in forward]
        low = lax.ppermute(
            lax.slice_in_dim(block, block.shape[dim] - width, None, axis=dim), axis, forward
        )
        high = lax.ppermute(lax.slice_in_dim(block, 0, width, axis=dim), axis, backward)
        block = jnp.concatenate([low, block, high], axis=dim)
    return block


def rotated(values, positions):
    half_dim = values.shape[-1] // 2
    inverse = ROPE_BASE ** (-2.0 * jnp.arange(half_dim, dtype=jnp.float32) / values.shape[-1])
    angles = positions.astype(jnp.float32)[:, None] * inverse[None, :]
    cosine = jnp.cos(angles)[:, None, :]
    sine = jnp.sin(angles)[:, None, :]
    first_half = values[..., :half_dim]
    second_half = values[..., half_dim:]
    return jnp.concatenate(
        [first_half * cosine - second_half * sine, first_half * sine + second_half * cosine],
        axis=-1,
    )


def body(
    tokens,
    norm_gain,
    att_query,
    att_key,
    att_value,
    ret_query,
    ret_key,
    ret_value,
    ret_gate,
    att_sink,
    decay_log,
    init_state,
    out_att,
    out_ret,
):
    tok_rows = tokens.shape[0]
    chan_local = tokens.shape[1]
    query_cols = att_query.shape[1]
    kv_cols = att_key.shape[1]
    rk_cols = ret_query.shape[1]
    rv_cols = ret_value.shape[1]
    heads_local = att_sink.shape[0]
    kv_local = kv_cols // HD
    groups = heads_local // kv_local
    ret_local = decay_log.shape[0]
    seq_offset = lax.axis_index("sp") * tok_rows
    seq_len = tok_rows * lax.axis_size("sp")
    joined = jnp.concatenate(
        [att_query, att_key, att_value, ret_query, ret_key, ret_value, ret_gate], axis=1
    )
    piece_f = lax.all_gather(tokens, "tp", axis=1, tiled=True).astype(jnp.float32)
    scaled = (piece_f * norm_gain[None, :]).astype(jnp.bfloat16)
    proj_sums = jnp.dot(scaled, joined, preferred_element_type=jnp.float32)
    squares = jnp.sum(piece_f * piece_f, axis=1)
    inv_rms = lax.rsqrt(squares / (chan_local * lax.axis_size("tp")) + NORM_EPS)
    projected = (proj_sums * inv_rms[:, None]).astype(jnp.bfloat16)
    off_rq = query_cols + 2 * kv_cols
    off_rk = off_rq + rk_cols
    off_rv = off_rk + rk_cols
    off_gate = off_rv + rv_cols
    key_vals = projected[:, query_cols:off_rq]
    padded = padded_2(key_vals, (("sp", 0),), WINDOW)
    block_rows = min(512, tok_rows)
    span_rows = block_rows + 2 * WINDOW
    queries = projected[:, :query_cols].reshape(tok_rows, kv_local, groups, HD)
    sink_col = att_sink.reshape(kv_local, groups, 1, 1)
    outputs = []
    for first_row in range(0, tok_rows, block_rows):
        query_block = queries[first_row : first_row + block_rows]
        span_block = padded[first_row : first_row + span_rows]
        key_block = span_block[:, :kv_cols].reshape(span_rows, kv_local, HD)
        value_block = span_block[:, kv_cols:].reshape(span_rows, kv_local, HD)
        scores = jnp.einsum(
            "qkgd,skd->kgqs", query_block, key_block, preferred_element_type=jnp.float32
        ) * HD ** (-0.5)
        query_pos = seq_offset + first_row + jnp.arange(block_rows, dtype=jnp.int32)
        key_pos = seq_offset + first_row - WINDOW + jnp.arange(span_rows, dtype=jnp.int32)
        allowed = (
            (jnp.abs(query_pos[:, None] - key_pos[None, :]) <= WINDOW)
            & (key_pos >= 0)[None, :]
            & (key_pos < seq_len)[None, :]
        )
        scores = jnp.where(allowed, scores, -jnp.inf)
        row_top = jnp.maximum(jnp.max(scores, axis=-1, keepdims=True), sink_col)
        raised = jnp.exp(scores - row_top)
        denominator = jnp.sum(raised, axis=-1, keepdims=True) + jnp.exp(sink_col - row_top)
        weights_bf = (raised / denominator).astype(jnp.bfloat16)
        block_out = jnp.einsum(
            "kgqs,skd->qkgd", weights_bf, value_block, preferred_element_type=jnp.float32
        )
        outputs.append(block_out.reshape(block_rows, query_cols).astype(jnp.bfloat16))
    attended = jnp.concatenate(outputs, axis=0)
    positions = seq_offset + jnp.arange(tok_rows, dtype=jnp.int32)
    query_rot = rotated(
        projected[:, off_rq:off_rk].astype(jnp.float32).reshape(tok_rows, ret_local, RK), positions
    )
    key_rot = rotated(
        projected[:, off_rk:off_rv].astype(jnp.float32).reshape(tok_rows, ret_local, RK), positions
    ) * RK ** (-0.5)
    value_f = projected[:, off_rv:off_gate].astype(jnp.float32).reshape(tok_rows, ret_local, RV)
    gate_f = projected[:, off_gate:].astype(jnp.float32)
    block_count = tok_rows // RET_BLOCK

    def heads_first(values, width):
        return jnp.transpose(values.reshape(block_count, RET_BLOCK, ret_local, width), (2, 0, 1, 3))

    query_h = heads_first(query_rot, RK)
    key_h = heads_first(key_rot, RK)
    value_h = heads_first(value_f, RV)
    block_logs = decay_log.reshape(ret_local, block_count, RET_BLOCK)
    cumul = jnp.cumsum(block_logs, axis=-1)
    block_log = cumul[..., -1]
    inner_w = jnp.einsum("hbnk,hbmk->hbnm", query_h, key_h, precision=HIGHEST) * jnp.exp(
        -jnp.abs(cumul[..., :, None] - cumul[..., None, :])
    )
    local_out = jnp.einsum("hbnm,hbmv->hbnv", inner_w, value_h, precision=HIGHEST)
    fwd_terms = jnp.einsum(
        "hbmk,hbmv->bhkv",
        key_h * jnp.exp(block_log[..., None] - cumul)[..., None],
        value_h,
        precision=HIGHEST,
    )
    bwd_terms = jnp.einsum(
        "hbmk,hbmv->bhkv", key_h * jnp.exp(cumul)[..., None], value_h, precision=HIGHEST
    )
    my_index = lax.axis_index("sp")
    axis_count = lax.axis_size("sp")
    upto = jnp.cumsum(block_log, axis=1)
    before_log = upto - block_log
    total_log = upto[:, -1:]
    after_log = total_log - upto
    order = jnp.arange(block_count)
    earlier = order[None, :] < order[:, None]
    fwd_w = jnp.where(earlier, jnp.exp(jnp.where(earlier, before_log[:, :, None] - upto[:, None, :], 0.0)), 0.0)
    later = order[None, :] > order[:, None]
    bwd_w = jnp.where(later, jnp.exp(jnp.where(later, before_log[:, None, :] - upto[:, :, None], 0.0)), 0.0)
    fwd_local = jnp.einsum("hba,ahkv->bhkv", fwd_w, fwd_terms, precision=HIGHEST)
    bwd_local = jnp.einsum("hba,ahkv->bhkv", bwd_w, bwd_terms, precision=HIGHEST)
    fwd_total = jnp.einsum("ha,ahkv->hkv", jnp.exp(after_log), fwd_terms, precision=HIGHEST)
    bwd_total = jnp.einsum("ha,ahkv->hkv", jnp.exp(before_log), bwd_terms, precision=HIGHEST)
    totals = lax.all_gather(jnp.stack([fwd_total, bwd_total]).astype(jnp.bfloat16), "sp").astype(jnp.float32)
    logs = lax.all_gather(total_log[:, 0], "sp")
    dev = jnp.arange(axis_count)
    dev_upto = jnp.cumsum(logs, axis=0)
    dev_before = dev_upto - logs
    mine_before = lax.dynamic_index_in_dim(dev_before, my_index, 0)
    mine_upto = lax.dynamic_index_in_dim(dev_upto, my_index, 0)
    is_low = (dev < my_index)[:, None]
    is_high = (dev > my_index)[:, None]
    low_w = jnp.where(is_low, jnp.exp(jnp.where(is_low, mine_before - dev_upto, 0.0)), 0.0)
    high_w = jnp.where(is_high, jnp.exp(jnp.where(is_high, dev_before - mine_upto, 0.0)), 0.0)
    fwd_start = jnp.einsum("dh,dhkv->hkv", low_w, totals[:, 0], precision=HIGHEST) + jnp.exp(mine_before[0])[:, None, None] * init_state[0]
    bwd_start = jnp.einsum("dh,dhkv->hkv", high_w, totals[:, 1], precision=HIGHEST) + jnp.exp(dev_upto[-1] - mine_upto[0])[:, None, None] * init_state[1]
    fwd_in = fwd_local + jnp.exp(before_log).T[:, :, None, None] * fwd_start[None]
    bwd_in = bwd_local + jnp.exp(after_log).T[:, :, None, None] * bwd_start[None]
    cross_out = jnp.exp(cumul)[..., None] * jnp.einsum(
        "hbnk,bhkv->hbnv", query_h, fwd_in, precision=HIGHEST
    )
    cross_out = cross_out + jnp.exp(block_log[..., None] - cumul)[..., None] * jnp.einsum(
        "hbnk,bhkv->hbnv", query_h, bwd_in, precision=HIGHEST
    )
    combined = local_out + cross_out
    centered = combined - jnp.mean(combined, axis=-1, keepdims=True)
    normed = centered * lax.rsqrt(jnp.mean(centered * centered, axis=-1, keepdims=True) + NORM_EPS)
    retained = jnp.transpose(normed, (1, 2, 0, 3)).reshape(tok_rows, ret_local * RV)
    ret_out = (jax.nn.silu(gate_f) * retained).astype(jnp.bfloat16)
    contract_dims = (((0,), (1,)), ((), ()))
    att_part = lax.dot_general(out_att, attended, contract_dims, preferred_element_type=jnp.float32)
    summed = lax.psum_scatter(
        (
            att_part
            + lax.dot_general(out_ret, ret_out, contract_dims, preferred_element_type=jnp.float32)
        ).astype(jnp.bfloat16),
        "tp",
        scatter_dimension=0,
        tiled=True,
    ).astype(jnp.float32)
    return summed.T.astype(jnp.bfloat16)


def solution(mesh):
    in_specs = (
        P("sp", "tp"),
        P(),
        P(None, "tp"),
        P(None, "tp"),
        P(None, "tp"),
        P(None, "tp"),
        P(None, "tp"),
        P(None, "tp"),
        P(None, "tp"),
        P("tp"),
        P("tp", "sp"),
        P(None, "tp", None, None),
        P("tp", None),
        P("tp", None),
    )
    out_specs = P("sp", "tp")
    return jax.shard_map(body, mesh=mesh, in_specs=in_specs, out_specs=out_specs, check_vma=False)
```

```python
import functools

import jax
import jax.numpy as jnp
import numpy as np
from jax import lax
from jax.experimental import pallas as pl
from jax.experimental.pallas import tpu as pltpu
from jax.sharding import PartitionSpec as P

HD = 64
RK = 64
RV = 128
WINDOW = 128
CHUNK = 256
NORM_EPS = 1e-06
ROPE_BASE = 10000.0
F32 = jnp.float32
BF16 = jnp.bfloat16
MESH = pl.DeviceIdType.MESH


def rope_tables(count, step, heads):
    half = RK // 2
    inverse = ROPE_BASE ** (-2.0 * np.arange(half, dtype=np.float64) / RK)
    angles = (np.arange(count, dtype=np.float64) * step)[:, None] * inverse[None, :]
    wide = np.tile(np.concatenate([angles, angles], axis=1), (1, heads))
    return np.cos(wide).astype(np.float32), np.sin(wide).astype(np.float32)


def remote(src, dst, send, recv, **where):
    return pltpu.make_async_remote_copy(
        src_ref=src, dst_ref=dst, send_sem=send, recv_sem=recv,
        device_id=where, device_id_type=MESH,
    )


def rows_of(index, size):
    return pl.ds(pl.multiple_of(index * size, size), size)


def mm(a, b):
    return jnp.dot(a, b, preferred_element_type=F32)


def mm_t(a, b):
    return lax.dot_general(a, b, (((1,), (1,)), ((), ())), preferred_element_type=F32)


def tm_m(a, b):
    return lax.dot_general(a, b, (((0,), (0,)), ((), ())), preferred_element_type=F32)


def kernel(cfg, *refs):
    (tokens, gain, w_q, w_k, w_v, w_rq, w_rk, w_rv, w_rg, sink, decay, init, o_att, o_ret,
     outer_cos, outer_sin, inner_cos, inner_sin, out) = refs[:19]
    n_buf = len(cfg["buffers"])
    w_bufs = refs[19:19 + n_buf]
    (w_out, gath, xbuf, qs, kbuf, vbuf, att, qfb, rloc, gs, fterm, bterm, blog, tot_f, tot_b,
     tots, logs, states, acc, s_part, r_part, s_cross, r_cross,
     w_sem, wo_sem, tok_sem, ag_send, ag_recv, halo_send, halo_recv, tot_send, tot_recv,
     log_send, log_recv, part_send, part_recv, cross_send, cross_recv) = refs[19 + n_buf:]
    n_tp, n_sp, n_chips, chunks = cfg["n_tp"], cfg["n_sp"], cfg["n_chips"], cfg["chunks"]
    chan, heads, ret, kv = cfg["chan"], cfg["heads"], cfg["ret"], cfg["kv"]
    rows = chunks * CHUNK
    width = n_tp * chan
    groups = heads // kv
    seq_len = rows * n_sp
    sp = lax.axis_index("sp")
    tp = lax.axis_index("tp")
    core = lax.rem(tp, 2)
    chip = lax.div(tp, 2)
    partner = chip * 2 + 1 - core

    def across(k):
        return lax.rem(chip + k, n_chips) * 2 + core

    token_copy = pltpu.make_async_copy(tokens, gath.at[tp], tok_sem)
    token_copy.start()
    weights = (w_q, w_k, w_v, w_rq, w_rk, w_rv, w_rg)
    w_copies = []
    for i, (w_ref, (b, off, cols)) in enumerate(zip(weights, cfg["places"])):
        dst = w_bufs[b].at[:, pl.ds(off, cols)] if cfg["joined"] else w_bufs[b]
        w_copies.append(pltpu.make_async_copy(w_ref, dst, w_sem.at[i]))
    for copy in w_copies:
        copy.start()
    o_copies = []
    half_rows = heads * HD
    for j in range(n_tp):
        for part, (src, first, count) in enumerate(
            ((o_att, 0, half_rows), (o_ret, half_rows, ret * RV))
        ):
            o_copies.append(pltpu.make_async_copy(
                src.at[:, pl.ds(j * chan, chan)], w_out.at[j, pl.ds(first, count), :],
                wo_sem.at[j, part]))
    for copy in o_copies:
        copy.start()

    barrier = pltpu.get_barrier_semaphore()
    for k in range(1, n_tp):
        pl.semaphore_signal(barrier, inc=1, device_id={"tp": lax.rem(tp + k, n_tp)}, device_id_type=MESH)
    for k in range(1, n_sp):
        pl.semaphore_signal(barrier, inc=1, device_id={"sp": lax.rem(sp + k, n_sp)}, device_id_type=MESH)
    pl.semaphore_wait(barrier, n_tp - 1 + n_sp - 1)

    def own_cross(c, k):
        return remote(tokens.at[rows_of(c, CHUNK), :], gath.at[tp, rows_of(c, CHUNK), :],
                      ag_send.at[k, c], ag_recv.at[tp, c], tp=across(k))

    def own_part(c):
        return remote(tokens.at[rows_of(c, CHUNK), :], gath.at[tp, rows_of(c, CHUNK), :],
                      ag_send.at[0, c], ag_recv.at[tp, c], tp=partner)

    def arrival(c, slot, k=0):
        return remote(gath.at[slot, rows_of(c, CHUNK), :], gath.at[slot, rows_of(c, CHUNK), :],
                      ag_send.at[k, c], ag_recv.at[slot, c], tp=partner)

    def start_sends(c, carry):
        for k in range(1, n_chips):
            own_cross(c, k).start()
        own_part(c).start()
        return carry

    lax.fori_loop(0, chunks, start_sends, 0)

    for h in range(ret):
        total = jnp.sum(decay[h:h + 1, :], axis=1, keepdims=True)
        logs[sp, h] = jnp.broadcast_to(total, (8, 128))

    def log_copy(k):
        return remote(logs.at[sp], logs.at[sp], log_send.at[k], log_recv.at[sp],
                      sp=lax.rem(sp + k, n_sp))

    def log_arrival(k):
        other = lax.rem(sp + k, n_sp)
        return remote(logs.at[other], logs.at[other], log_send.at[k], log_recv.at[other], sp=other)

    token_copy.wait()
    for copy in w_copies:
        copy.wait()

    row_i = lax.broadcasted_iota(jnp.int32, (CHUNK, CHUNK), 0)
    col_i = lax.broadcasted_iota(jnp.int32, (CHUNK, CHUNK), 1)
    rw = ret * RK
    p_row = lax.broadcasted_iota(jnp.int32, (rw, rw), 0)
    p_col = lax.broadcasted_iota(jnp.int32, (rw, rw), 1)
    first_half = lax.rem(p_col, RK) < RK // 2
    swap = jnp.where(
        first_half & (p_row == p_col + RK // 2), -1.0,
        jnp.where(jnp.logical_not(first_half) & (p_row == p_col - RK // 2), 1.0, 0.0),
    ).astype(BF16)

    def attend(i):
        here = rows_of(i, 128)
        span = pl.ds(pl.multiple_of(i * 128, 128), 128 + 2 * WINDOW)
        shape = (128, 128 + 2 * WINDOW)
        q_i = lax.broadcasted_iota(jnp.int32, shape, 0)
        k_i = lax.broadcasted_iota(jnp.int32, shape, 1)
        key_pos = k_i + (sp * rows + i * 128 - WINDOW)
        allowed = (k_i >= q_i) & (k_i <= q_i + 2 * WINDOW) & (key_pos >= 0) & (key_pos < seq_len)
        allowed = jnp.concatenate([allowed.astype(F32)] * groups, axis=0) > 0.5
        done = []
        for g in range(kv):
            query = jnp.concatenate(
                [qs[here, (g * groups + j) * HD:(g * groups + j + 1) * HD] for j in range(groups)], axis=0)
            key = kbuf[span, g * HD:(g + 1) * HD]
            value = vbuf[span, g * HD:(g + 1) * HD]
            scores = jnp.where(allowed, mm_t(query, key), -jnp.inf)
            sink_col = jnp.concatenate(
                [jnp.full((128, 1), sink[g * groups + j], F32) for j in range(groups)], axis=0)
            top = jnp.maximum(jnp.max(scores, axis=1, keepdims=True), sink_col)
            raised = jnp.exp(scores - top)
            denominator = jnp.sum(raised, axis=1, keepdims=True) + jnp.exp(sink_col - top)
            result = mm(raised.astype(BF16), value) / denominator
            for j in range(groups):
                done.append(result[j * 128:(j + 1) * 128])
        att[here, :] = jnp.concatenate(done, axis=1).astype(BF16)

    def chunk_body(c, carry):
        here = rows_of(c, CHUNK)
        for k in range(1, n_chips):
            slot = across(k)
            arrival(c, slot).wait_recv()
            arrival(c, slot, n_chips - 1 + k).start()
        arrival(c, partner).wait_recv()
        for k in range(1, n_chips):
            arrival(c, lax.rem(chip + k, n_chips) * 2 + 1 - core).wait_recv()
        squares = jnp.zeros((CHUNK, 1), F32)
        for s in range(n_tp):
            piece = gath[s, here, :].astype(F32)
            squares = squares + jnp.sum(piece * piece, axis=1, keepdims=True)
            xbuf[:, s * chan:(s + 1) * chan] = (piece * gain[0:1, s * chan:(s + 1) * chan]).astype(BF16)
        inv_rms = lax.rsqrt(squares / width + NORM_EPS)
        found = {}
        for b, first, cols, names in cfg["dots"]:
            block = (mm(xbuf[...], w_bufs[b][:, first:first + cols]) * inv_rms).astype(BF16)
            at = 0
            for name, count in names:
                found[name] = block[:, at:at + count]
                at += count
        qs[here, :] = found["q"] * jnp.asarray(HD ** -0.5, BF16)
        shifted = pl.ds(pl.multiple_of(c * CHUNK + WINDOW, 128), CHUNK)
        kbuf[shifted, :] = found["k"]
        vbuf[shifted, :] = found["v"]
        gs[here, :] = found["g"]
        place = sp * chunks + c
        oc, os_ = outer_cos[pl.ds(place, 1), :], outer_sin[pl.ds(place, 1), :]
        ic, is_ = inner_cos[...], inner_sin[...]
        cosine = oc * ic - os_ * is_
        sine = os_ * ic + oc * is_
        query_rot = found["rq"].astype(F32) * cosine + mm(found["rq"], swap) * sine
        key_rot = (found["rk"].astype(F32) * cosine + mm(found["rk"], swap) * sine) * RK ** -0.5
        for h in range(ret):
            log_row = decay[h:h + 1, here]
            wide = jnp.broadcast_to(log_row, (CHUNK, CHUNK))
            log_col = jnp.sum(jnp.where(row_i == col_i, wide, 0.0), axis=1, keepdims=True)
            cum_col = jnp.sum(jnp.where(col_i <= row_i, wide, 0.0), axis=1, keepdims=True)
            cum_row = jnp.sum(jnp.where(row_i <= col_i, log_col, 0.0), axis=0, keepdims=True)
            total = jnp.sum(log_row, axis=1, keepdims=True)
            query = query_rot[:, h * RK:(h + 1) * RK]
            key = key_rot[:, h * RK:(h + 1) * RK]
            value = found["rv"][:, h * RV:(h + 1) * RV]
            inner = mm_t(query.astype(BF16), key.astype(BF16)) * jnp.exp(-jnp.abs(cum_col - cum_row))
            rloc[h, here, :] = mm(inner.astype(BF16), value)
            up = jnp.exp(cum_col)
            down = jnp.exp(jnp.minimum(total - cum_col, 0.0))
            qfb[h, here, :] = jnp.concatenate([query * up, query * down], axis=1).astype(BF16)
            both = jnp.concatenate([key * down, key * up], axis=1).astype(BF16)
            terms = tm_m(both, value)
            fterm[h, c] = terms[:RK]
            bterm[h, c] = terms[RK:]
            blog[h, c] = jnp.broadcast_to(total, (8, 128))

        @pl.when(c > 0)
        def _():
            attend(2 * c - 1)
            attend(2 * c)

        @pl.when(c == 0)
        def _():
            for k in range(1, n_sp):
                log_copy(k).start()

        return carry

    lax.fori_loop(0, chunks, chunk_body, 0)

    for h in range(ret):
        state = jnp.zeros((RK, RV), F32)
        back = jnp.zeros((RK, RV), F32)
        for c in range(chunks):
            state = jnp.exp(blog[h, c, 0:1, :]) * state + fterm[h, c]
            back = jnp.exp(blog[h, chunks - 1 - c, 0:1, :]) * back + bterm[h, chunks - 1 - c]
        tot_f[h] = state.astype(BF16)
        tot_b[h] = back.astype(BF16)

    left = lax.rem(sp + n_sp - 1, n_sp)
    right = lax.rem(sp + 1, n_sp)
    halos = []
    for i, buf in enumerate((kbuf, vbuf)):
        halos.append(remote(buf.at[pl.ds(rows, WINDOW), :], buf.at[pl.ds(0, WINDOW), :],
                            halo_send.at[0, i], halo_recv.at[0, i], sp=right))
        halos.append(remote(buf.at[pl.ds(WINDOW, WINDOW), :], buf.at[pl.ds(rows + WINDOW, WINDOW), :],
                            halo_send.at[1, i], halo_recv.at[1, i], sp=left))
    for copy in halos:
        copy.start()

    def send_f(d, carry):
        remote(tot_f, tots.at[sp], tot_send.at[d], tot_recv.at[sp], sp=d).start()
        return carry

    def send_b(d, carry):
        remote(tot_b, tots.at[sp], tot_send.at[d], tot_recv.at[sp], sp=d).start()
        return carry

    lax.fori_loop(sp + 1, n_sp, send_f, 0)
    lax.fori_loop(0, sp, send_b, 0)

    for copy in halos:
        copy.wait()
    attend(0)
    attend(2 * chunks - 1)
    for copy in o_copies:
        copy.wait()

    for k in range(1, n_sp):
        log_arrival(k).wait_recv()

    def total_arrival(e):
        return remote(tots.at[e], tots.at[e], tot_send.at[e], tot_recv.at[e], sp=e)

    for h in range(ret):
        states[0, h] = init[0, h]
        states[1, h] = init[1, h]

    def from_low(e, carry):
        total_arrival(e).wait_recv()
        for h in range(ret):
            states[0, h] = jnp.exp(logs[e, h, 0:1, :]) * states[0, h] + tots[e, h].astype(F32)
        return carry

    def from_high(i, carry):
        e = n_sp - 1 - i
        total_arrival(e).wait_recv()
        for h in range(ret):
            states[1, h] = jnp.exp(logs[e, h, 0:1, :]) * states[1, h] + tots[e, h].astype(F32)
        return carry

    lax.fori_loop(0, sp, from_low, 0)
    lax.fori_loop(0, n_sp - 1 - sp, from_high, 0)

    for h in range(ret):
        state = states[0, h]
        back = states[1, h]
        for c in range(chunks):
            term = fterm[h, c]
            fterm[h, c] = state
            state = jnp.exp(blog[h, c, 0:1, :]) * state + term
            r = chunks - 1 - c
            term = bterm[h, r]
            bterm[h, r] = back
            back = jnp.exp(blog[h, r, 0:1, :]) * back + term

    def part_copy(k, c):
        return remote(s_part.at[k, rows_of(c, CHUNK), :], r_part.at[k, rows_of(c, CHUNK), :],
                      part_send.at[k, c], part_recv.at[k, c], tp=partner)

    def cross_copy(k, c):
        return remote(s_cross.at[k - 1, rows_of(c, CHUNK), :],
                      r_cross.at[n_chips - k - 1, rows_of(c, CHUNK), :],
                      cross_send.at[k - 1, c], cross_recv.at[n_chips - k - 1, c], tp=across(k))

    def project(c):
        here = rows_of(c, CHUNK)
        pieces = [att[here, :]]
        for h in range(ret):
            both = jnp.concatenate([fterm[h, c], bterm[h, c]], axis=0).astype(BF16)
            combined = rloc[h, here, :] + mm(qfb[h, here, :], both)
            centered = combined - jnp.mean(combined, axis=1, keepdims=True)
            normed = centered * lax.rsqrt(jnp.mean(centered * centered, axis=1, keepdims=True) + NORM_EPS)
            gate = gs[here, h * RV:(h + 1) * RV].astype(F32)
            pieces.append((gate / (1.0 + jnp.exp(-gate)) * normed).astype(BF16))
        mixed = jnp.concatenate(pieces, axis=1)
        for k in list(range(1, n_chips)) + [0]:
            owner = lax.rem(chip + k, n_chips) * 2
            s_part[k, here, :] = mm(mixed, w_out[owner + 1 - core]).astype(BF16)
            acc[k, here, :] = mm(mixed, w_out[owner + core])
            part_copy(k, c).start()

    def relay(c):
        here = rows_of(c, CHUNK)
        for k in range(1, n_chips):
            part_copy(k, c).wait_recv()
            s_cross[k - 1, here, :] = (acc[k, here, :] + r_part[k, here, :].astype(F32)).astype(BF16)
            cross_copy(k, c).start()

    def mix_body(c, carry):
        @pl.when(c < chunks)
        def _():
            project(c)

        @pl.when(c > 0)
        def _():
            relay(c - 1)

        return carry

    lax.fori_loop(0, chunks + 1, mix_body, 0)

    def last_body(c, carry):
        here = rows_of(c, CHUNK)
        part_copy(0, c).wait_recv()
        total = acc[0, here, :] + r_part[0, here, :].astype(F32)
        for k in range(1, n_chips):
            cross_copy(k, c).wait_recv()
        for k in range(1, n_chips):
            total = total + r_cross[k - 1, here, :].astype(F32)
        out[here, :] = total.astype(BF16)
        return carry

    lax.fori_loop(0, chunks, last_body, 0)

    def sent(c, carry):
        own_part(c).wait_send()
        for k in range(1, n_chips):
            own_cross(c, k).wait_send()
            arrival(c, across(k), n_chips - 1 + k).wait_send()
            cross_copy(k, c).wait_send()
        for k in range(n_chips):
            part_copy(k, c).wait_send()
        return carry

    lax.fori_loop(0, chunks, sent, 0)
    for k in range(1, n_sp):
        log_copy(k).wait_send()

    def sent_total(d, carry):
        total_arrival(d).wait_send()
        return carry

    lax.fori_loop(sp + 1, n_sp, sent_total, 0)
    lax.fori_loop(0, sp, sent_total, 0)


def body(n_sp, n_tp, tokens, norm_gain, w_q, w_k, w_v, w_rq, w_rk, w_rv, w_rg, att_sink,
         decay_log, init_state, out_att, out_ret):
    rows, chan = tokens.shape
    width = n_tp * chan
    ret = decay_log.shape[0]
    heads = att_sink.shape[0]
    kv_cols = w_k.shape[1]
    kv = kv_cols // HD
    chunks = rows // CHUNK
    n_chips = n_tp // 2
    weights = (w_q, w_k, w_v, w_rq, w_rk, w_rv, w_rg)
    names = ("q", "k", "v", "rq", "rk", "rv", "g")
    cols = [w.shape[1] for w in weights]
    joined = all(count % 128 == 0 for count in cols)
    places, dots = [], []
    if joined:
        buffers = [sum(cols)]
        at = 0
        for count in cols:
            places.append((0, at, count))
            at += count
        for group in ((0,), (1, 2), (3, 4), (5,), (6,)):
            dots.append((0, places[group[0]][1], sum(cols[i] for i in group),
                         tuple((names[i], cols[i]) for i in group)))
    else:
        buffers = cols
        for i, count in enumerate(cols):
            places.append((i, 0, count))
            dots.append((i, 0, count, ((names[i], count),)))
    cfg = dict(n_sp=n_sp, n_tp=n_tp, n_chips=n_chips, chunks=chunks, chan=chan, heads=heads,
               ret=ret, kv=kv, buffers=buffers, places=places, dots=dots, joined=joined)
    outer = rope_tables(n_sp * chunks, CHUNK, ret)
    inner = rope_tables(CHUNK, 1, ret)
    vmem = pl.BlockSpec(memory_space=pltpu.VMEM)
    anyw = pl.BlockSpec(memory_space=pl.ANY)
    smem = pl.BlockSpec(memory_space=pltpu.SMEM)
    dma = pltpu.SemaphoreType.DMA
    mixed_rows = heads * HD + ret * RV
    others = max(n_chips - 1, 1)
    scratch = [pltpu.VMEM((width, count), BF16) for count in buffers] + [
        pltpu.VMEM((n_tp, mixed_rows, chan), BF16),
        pltpu.VMEM((n_tp, rows, chan), BF16),
        pltpu.VMEM((CHUNK, width), BF16),
        pltpu.VMEM((rows, heads * HD), BF16),
        pltpu.VMEM((rows + 2 * WINDOW, kv_cols), BF16),
        pltpu.VMEM((rows + 2 * WINDOW, kv_cols), BF16),
        pltpu.VMEM((rows, heads * HD), BF16),
        pltpu.VMEM((ret, rows, 2 * RK), BF16),
        pltpu.VMEM((ret, rows, RV), F32),
        pltpu.VMEM((rows, ret * RV), BF16),
        pltpu.VMEM((ret, chunks, RK, RV), F32),
        pltpu.VMEM((ret, chunks, RK, RV), F32),
        pltpu.VMEM((ret, chunks, 8, 128), F32),
        pltpu.VMEM((ret, RK, RV), BF16),
        pltpu.VMEM((ret, RK, RV), BF16),
        pltpu.VMEM((n_sp, ret, RK, RV), BF16),
        pltpu.VMEM((n_sp, ret, 8, 128), F32),
        pltpu.VMEM((2, ret, RK, RV), F32),
        pltpu.VMEM((n_chips, rows, chan), F32),
        pltpu.VMEM((n_chips, rows, chan), BF16),
        pltpu.VMEM((n_chips, rows, chan), BF16),
        pltpu.VMEM((others, rows, chan), BF16),
        pltpu.VMEM((others, rows, chan), BF16),
        dma((7,)), dma((n_tp, 2)), dma,
        dma((2 * n_chips, chunks)), dma((n_tp, chunks)),
        dma((2, 2)), dma((2, 2)),
        dma((n_sp,)), dma((n_sp,)),
        dma((n_sp,)), dma((n_sp,)),
        dma((n_chips, chunks)), dma((n_chips, chunks)),
        dma((others, chunks)), dma((others, chunks)),
    ]
    return pl.pallas_call(
        functools.partial(kernel, cfg),
        out_shape=jax.ShapeDtypeStruct((rows, chan), BF16),
        in_specs=[anyw, vmem] + [anyw] * 7 + [smem, vmem, vmem, anyw, anyw] + [vmem] * 4,
        out_specs=vmem,
        scratch_shapes=scratch,
        compiler_params=pltpu.CompilerParams(
            collective_id=0, has_side_effects=True, vmem_limit_bytes=60 * 1024 * 1024),
    )(tokens, norm_gain.reshape(1, width), *weights, att_sink, decay_log, init_state,
      out_att, out_ret, *(jnp.asarray(t) for t in outer), *(jnp.asarray(t) for t in inner))


def solution(mesh):
    n_sp, n_tp = mesh.shape["sp"], mesh.shape["tp"]
    in_specs = (
        P("sp", "tp"),
        P(),
        P(None, "tp"),
        P(None, "tp"),
        P(None, "tp"),
        P(None, "tp"),
        P(None, "tp"),
        P(None, "tp"),
        P(None, "tp"),
        P("tp"),
        P("tp", "sp"),
        P(None, "tp", None, None),
        P("tp", None),
        P("tp", None),
    )
    return jax.shard_map(functools.partial(body, n_sp, n_tp), mesh=mesh, in_specs=in_specs,
                         out_specs=P("sp", "tp"), check_vma=False)
```

```python
import functools

import jax
import jax.numpy as jnp
import numpy as np
from jax import lax
from jax.experimental import pallas as pl
from jax.experimental.pallas import tpu as pltpu
from jax.sharding import PartitionSpec as P

HD = 64
RK = 64
RV = 128
WINDOW = 128
CHUNK = 256
MIX = 128
NORM_EPS = 1e-06
ROPE_BASE = 10000.0
F32 = jnp.float32
BF16 = jnp.bfloat16
MESH = pl.DeviceIdType.MESH


def rope_tables(count, step, heads):
    half = RK // 2
    inverse = ROPE_BASE ** (-2.0 * np.arange(half, dtype=np.float64) / RK)
    angles = (np.arange(count, dtype=np.float64) * step)[:, None] * inverse[None, :]
    wide = np.tile(np.concatenate([angles, angles], axis=1), (1, heads))
    return np.cos(wide).astype(np.float32), np.sin(wide).astype(np.float32)


def remote(src, dst, send, recv, **where):
    return pltpu.make_async_remote_copy(
        src_ref=src, dst_ref=dst, send_sem=send, recv_sem=recv,
        device_id=where, device_id_type=MESH,
    )


def rows_of(index, size):
    return pl.ds(pl.multiple_of(index * size, size), size)


def mm(a, b):
    return jnp.dot(a, b, preferred_element_type=F32)


def mm_t(a, b):
    return lax.dot_general(a, b, (((1,), (1,)), ((), ())), preferred_element_type=F32)


def tm_m(a, b):
    return lax.dot_general(a, b, (((0,), (0,)), ((), ())), preferred_element_type=F32)


def kernel(cfg, *refs):
    (tokens, gain, w_q, w_k, w_v, w_rq, w_rk, w_rv, w_rg, sink, decay, init, o_att, o_ret,
     outer_cos, outer_sin, inner_cos, inner_sin, out) = refs[:19]
    n_buf = len(cfg["buffers"])
    w_bufs = refs[19:19 + n_buf]
    (w_out, gath, xbuf, qs, kbuf, vbuf, att, qfb, rloc, gs, fterm, bterm, blog, tot_f, tot_b,
     tots, logs, states, acc, s_part, r_part, s_cross, r_cross,
     w_sem, wo_sem, tok_sem, ag_send, ag_recv, halo_send, halo_recv, tot_send, tot_recv,
     log_send, log_recv, part_send, part_recv, cross_send, cross_recv) = refs[19 + n_buf:]
    n_tp, n_sp, n_chips, chunks = cfg["n_tp"], cfg["n_sp"], cfg["n_chips"], cfg["chunks"]
    chan, heads, ret, kv = cfg["chan"], cfg["heads"], cfg["ret"], cfg["kv"]
    rows = chunks * CHUNK
    width = n_tp * chan
    groups = heads // kv
    seq_len = rows * n_sp
    sp = lax.axis_index("sp")
    tp = lax.axis_index("tp")
    core = lax.rem(tp, 2)
    chip = lax.div(tp, 2)
    partner = chip * 2 + 1 - core

    def across(k):
        return lax.rem(chip + k, n_chips) * 2 + core

    token_copy = pltpu.make_async_copy(tokens, gath.at[tp], tok_sem)
    token_copy.start()
    weights = (w_q, w_k, w_v, w_rq, w_rk, w_rv, w_rg)
    w_copies = []
    for i, (w_ref, (b, off, cols)) in enumerate(zip(weights, cfg["places"])):
        dst = w_bufs[b].at[:, pl.ds(off, cols)] if cfg["joined"] else w_bufs[b]
        w_copies.append(pltpu.make_async_copy(w_ref, dst, w_sem.at[i]))
    for copy in w_copies:
        copy.start()
    o_copies = []
    half_rows = heads * HD
    for j in range(n_tp):
        for part, (src, first, count) in enumerate(
            ((o_att, 0, half_rows), (o_ret, half_rows, ret * RV))
        ):
            o_copies.append(pltpu.make_async_copy(
                src.at[:, pl.ds(j * chan, chan)], w_out.at[j, pl.ds(first, count), :],
                wo_sem.at[j, part]))
    for copy in o_copies:
        copy.start()

    barrier = pltpu.get_barrier_semaphore()
    for k in range(1, n_tp):
        pl.semaphore_signal(barrier, inc=1, device_id={"tp": lax.rem(tp + k, n_tp)}, device_id_type=MESH)
    for k in range(1, n_sp):
        pl.semaphore_signal(barrier, inc=1, device_id={"sp": lax.rem(sp + k, n_sp)}, device_id_type=MESH)
    pl.semaphore_wait(barrier, n_tp - 1 + n_sp - 1)

    def own_cross(c, k):
        return remote(tokens.at[rows_of(c, CHUNK), :], gath.at[tp, rows_of(c, CHUNK), :],
                      ag_send.at[k, c], ag_recv.at[tp, c], tp=across(k))

    def own_part(c):
        return remote(tokens.at[rows_of(c, CHUNK), :], gath.at[tp, rows_of(c, CHUNK), :],
                      ag_send.at[0, c], ag_recv.at[tp, c], tp=partner)

    def arrival(c, slot, k=0):
        return remote(gath.at[slot, rows_of(c, CHUNK), :], gath.at[slot, rows_of(c, CHUNK), :],
                      ag_send.at[k, c], ag_recv.at[slot, c], tp=partner)

    def start_sends(c, carry):
        for k in range(1, n_chips):
            own_cross(c, k).start()
        own_part(c).start()
        return carry

    lax.fori_loop(0, chunks, start_sends, 0)

    for h in range(ret):
        total = jnp.sum(decay[h:h + 1, :], axis=1, keepdims=True)
        logs[sp, h] = jnp.broadcast_to(total, (8, 128))

    def log_copy(k):
        return remote(logs.at[sp], logs.at[sp], log_send.at[k], log_recv.at[sp],
                      sp=lax.rem(sp + k, n_sp))

    def log_arrival(k):
        other = lax.rem(sp + k, n_sp)
        return remote(logs.at[other], logs.at[other], log_send.at[k], log_recv.at[other], sp=other)

    token_copy.wait()
    for copy in w_copies:
        copy.wait()

    row_i = lax.broadcasted_iota(jnp.int32, (CHUNK, CHUNK), 0)
    col_i = lax.broadcasted_iota(jnp.int32, (CHUNK, CHUNK), 1)
    rw = ret * RK
    p_row = lax.broadcasted_iota(jnp.int32, (rw, rw), 0)
    p_col = lax.broadcasted_iota(jnp.int32, (rw, rw), 1)
    first_half = lax.rem(p_col, RK) < RK // 2
    swap = jnp.where(
        first_half & (p_row == p_col + RK // 2), -1.0,
        jnp.where(jnp.logical_not(first_half) & (p_row == p_col - RK // 2), 1.0, 0.0),
    ).astype(BF16)

    def attend(i):
        here = rows_of(i, 128)
        span = pl.ds(pl.multiple_of(i * 128, 128), 128 + 2 * WINDOW)
        shape = (128, 128 + 2 * WINDOW)
        q_i = lax.broadcasted_iota(jnp.int32, shape, 0)
        k_i = lax.broadcasted_iota(jnp.int32, shape, 1)
        key_pos = k_i + (sp * rows + i * 128 - WINDOW)
        allowed = (k_i >= q_i) & (k_i <= q_i + 2 * WINDOW) & (key_pos >= 0) & (key_pos < seq_len)
        allowed = jnp.concatenate([allowed.astype(F32)] * groups, axis=0) > 0.5
        done = []
        for g in range(kv):
            query = jnp.concatenate(
                [qs[here, (g * groups + j) * HD:(g * groups + j + 1) * HD] for j in range(groups)], axis=0)
            key = kbuf[span, g * HD:(g + 1) * HD]
            value = vbuf[span, g * HD:(g + 1) * HD]
            scores = jnp.where(allowed, mm_t(query, key), -jnp.inf)
            sink_col = jnp.concatenate(
                [jnp.full((128, 1), sink[g * groups + j], F32) for j in range(groups)], axis=0)
            top = jnp.maximum(jnp.max(scores, axis=1, keepdims=True), sink_col)
            raised = jnp.exp(scores - top)
            denominator = jnp.sum(raised, axis=1, keepdims=True) + jnp.exp(sink_col - top)
            result = mm(raised.astype(BF16), value) / denominator
            for j in range(groups):
                done.append(result[j * 128:(j + 1) * 128])
        att[here, :] = jnp.concatenate(done, axis=1).astype(BF16)

    per = CHUNK // 128

    def chunk_body(c, carry):
        here = rows_of(c, CHUNK)
        for k in range(1, n_chips):
            slot = across(k)
            arrival(c, slot).wait_recv()
            arrival(c, slot, n_chips - 1 + k).start()
        for j in range(per):
            block = per * (c - 1) - 1 + j

            @pl.when(block > 0)
            def _():
                attend(block)

        arrival(c, partner).wait_recv()
        for k in range(1, n_chips):
            arrival(c, lax.rem(chip + k, n_chips) * 2 + 1 - core).wait_recv()
        squares = jnp.zeros((CHUNK, 1), F32)
        for s in range(n_tp):
            piece = gath[s, here, :].astype(F32)
            squares = squares + jnp.sum(piece * piece, axis=1, keepdims=True)
            xbuf[:, s * chan:(s + 1) * chan] = (piece * gain[0:1, s * chan:(s + 1) * chan]).astype(BF16)
        inv_rms = lax.rsqrt(squares / width + NORM_EPS)
        found = {}
        for b, first, cols, names in cfg["dots"]:
            block = (mm(xbuf[...], w_bufs[b][:, first:first + cols]) * inv_rms).astype(BF16)
            at = 0
            for name, count in names:
                found[name] = block[:, at:at + count]
                at += count
        qs[here, :] = found["q"] * jnp.asarray(HD ** -0.5, BF16)
        shifted = pl.ds(pl.multiple_of(c * CHUNK + WINDOW, 128), CHUNK)
        kbuf[shifted, :] = found["k"]
        vbuf[shifted, :] = found["v"]
        gs[here, :] = found["g"]
        place = sp * chunks + c
        oc, os_ = outer_cos[pl.ds(place, 1), :], outer_sin[pl.ds(place, 1), :]
        ic, is_ = inner_cos[...], inner_sin[...]
        cosine = oc * ic - os_ * is_
        sine = os_ * ic + oc * is_
        query_rot = found["rq"].astype(F32) * cosine + mm(found["rq"], swap) * sine
        key_rot = (found["rk"].astype(F32) * cosine + mm(found["rk"], swap) * sine) * RK ** -0.5
        for h in range(ret):
            log_row = decay[h:h + 1, here]
            wide = jnp.broadcast_to(log_row, (CHUNK, CHUNK))
            log_col = jnp.sum(jnp.where(row_i == col_i, wide, 0.0), axis=1, keepdims=True)
            cum_col = jnp.sum(jnp.where(col_i <= row_i, wide, 0.0), axis=1, keepdims=True)
            cum_row = jnp.sum(jnp.where(row_i <= col_i, log_col, 0.0), axis=0, keepdims=True)
            total = jnp.sum(log_row, axis=1, keepdims=True)
            query = query_rot[:, h * RK:(h + 1) * RK]
            key = key_rot[:, h * RK:(h + 1) * RK]
            value = found["rv"][:, h * RV:(h + 1) * RV]
            inner = mm_t(query.astype(BF16), key.astype(BF16)) * jnp.exp(-jnp.abs(cum_col - cum_row))
            rloc[h, here, :] = mm(inner.astype(BF16), value)
            up = jnp.exp(cum_col)
            down = jnp.exp(jnp.minimum(total - cum_col, 0.0))
            qfb[h, here, :] = jnp.concatenate([query * up, query * down], axis=1).astype(BF16)
            both = jnp.concatenate([key * down, key * up], axis=1).astype(BF16)
            terms = tm_m(both, value)
            fterm[h, c] = terms[:RK]
            bterm[h, c] = terms[RK:]
            blog[h, c] = jnp.broadcast_to(total, (8, 128))

        @pl.when(c == 0)
        def _():
            for k in range(1, n_sp):
                log_copy(k).start()

        return carry

    lax.fori_loop(0, chunks, chunk_body, 0)

    for h in range(ret):
        state = jnp.zeros((RK, RV), F32)
        back = jnp.zeros((RK, RV), F32)
        for c in range(chunks):
            state = jnp.exp(blog[h, c, 0:1, :]) * state + fterm[h, c]
            back = jnp.exp(blog[h, chunks - 1 - c, 0:1, :]) * back + bterm[h, chunks - 1 - c]
        tot_f[h] = state.astype(BF16)
        tot_b[h] = back.astype(BF16)

    left = lax.rem(sp + n_sp - 1, n_sp)
    right = lax.rem(sp + 1, n_sp)
    halos = []
    for i, buf in enumerate((kbuf, vbuf)):
        halos.append(remote(buf.at[pl.ds(rows, WINDOW), :], buf.at[pl.ds(0, WINDOW), :],
                            halo_send.at[0, i], halo_recv.at[0, i], sp=right))
        halos.append(remote(buf.at[pl.ds(WINDOW, WINDOW), :], buf.at[pl.ds(rows + WINDOW, WINDOW), :],
                            halo_send.at[1, i], halo_recv.at[1, i], sp=left))
    for copy in halos:
        copy.start()

    def send_f(d, carry):
        remote(tot_f, tots.at[sp], tot_send.at[d], tot_recv.at[sp], sp=d).start()
        return carry

    def send_b(d, carry):
        remote(tot_b, tots.at[sp], tot_send.at[d], tot_recv.at[sp], sp=d).start()
        return carry

    lax.fori_loop(sp + 1, n_sp, send_f, 0)
    lax.fori_loop(0, sp, send_b, 0)

    def late(i, carry):
        attend(i)
        return carry

    lax.fori_loop(max(per * (chunks - 1) - 1, 1), per * chunks - 1, late, 0)
    for copy in halos:
        copy.wait()
    attend(0)
    attend(per * chunks - 1)
    for copy in o_copies:
        copy.wait()

    for k in range(1, n_sp):
        log_arrival(k).wait_recv()

    def total_arrival(e):
        return remote(tots.at[e], tots.at[e], tot_send.at[e], tot_recv.at[e], sp=e)

    for h in range(ret):
        states[0, h] = init[0, h]
        states[1, h] = init[1, h]

    def from_low(e, carry):
        total_arrival(e).wait_recv()
        for h in range(ret):
            states[0, h] = jnp.exp(logs[e, h, 0:1, :]) * states[0, h] + tots[e, h].astype(F32)
        return carry

    def from_high(i, carry):
        e = n_sp - 1 - i
        total_arrival(e).wait_recv()
        for h in range(ret):
            states[1, h] = jnp.exp(logs[e, h, 0:1, :]) * states[1, h] + tots[e, h].astype(F32)
        return carry

    lax.fori_loop(0, sp, from_low, 0)
    lax.fori_loop(0, n_sp - 1 - sp, from_high, 0)

    for h in range(ret):
        state = states[0, h]
        back = states[1, h]
        for c in range(chunks):
            term = fterm[h, c]
            fterm[h, c] = state
            state = jnp.exp(blog[h, c, 0:1, :]) * state + term
            r = chunks - 1 - c
            term = bterm[h, r]
            bterm[h, r] = back
            back = jnp.exp(blog[h, r, 0:1, :]) * back + term

    mixes = rows // MIX

    def part_copy(k, c):
        return remote(s_part.at[k, rows_of(c, MIX), :], r_part.at[k, rows_of(c, MIX), :],
                      part_send.at[k, c], part_recv.at[k, c], tp=partner)

    def cross_copy(k, c):
        return remote(s_cross.at[k - 1, rows_of(c, MIX), :],
                      r_cross.at[n_chips - k - 1, rows_of(c, MIX), :],
                      cross_send.at[k - 1, c], cross_recv.at[n_chips - k - 1, c], tp=across(k))

    def project(c):
        here = rows_of(c, MIX)
        at = lax.div(c, CHUNK // MIX)
        pieces = [att[here, :]]
        for h in range(ret):
            both = jnp.concatenate([fterm[h, at], bterm[h, at]], axis=0).astype(BF16)
            combined = rloc[h, here, :] + mm(qfb[h, here, :], both)
            centered = combined - jnp.mean(combined, axis=1, keepdims=True)
            normed = centered * lax.rsqrt(jnp.mean(centered * centered, axis=1, keepdims=True) + NORM_EPS)
            gate = gs[here, h * RV:(h + 1) * RV].astype(F32)
            pieces.append((gate / (1.0 + jnp.exp(-gate)) * normed).astype(BF16))
        mixed = jnp.concatenate(pieces, axis=1)
        for k in list(range(1, n_chips)) + [0]:
            owner = lax.rem(chip + k, n_chips) * 2
            s_part[k, here, :] = mm(mixed, w_out[owner + 1 - core]).astype(BF16)
            acc[k, here, :] = mm(mixed, w_out[owner + core])
            part_copy(k, c).start()

    def relay(c):
        here = rows_of(c, MIX)
        for k in range(1, n_chips):
            part_copy(k, c).wait_recv()
            s_cross[k - 1, here, :] = (acc[k, here, :] + r_part[k, here, :].astype(F32)).astype(BF16)
            cross_copy(k, c).start()

    def mix_body(c, carry):
        @pl.when(c < mixes)
        def _():
            project(c)

        @pl.when(c > 0)
        def _():
            relay(c - 1)

        return carry

    lax.fori_loop(0, mixes + 1, mix_body, 0)

    def last_body(c, carry):
        here = rows_of(c, MIX)
        part_copy(0, c).wait_recv()
        total = acc[0, here, :] + r_part[0, here, :].astype(F32)
        for k in range(1, n_chips):
            cross_copy(k, c).wait_recv()
        for k in range(1, n_chips):
            total = total + r_cross[k - 1, here, :].astype(F32)
        out[here, :] = total.astype(BF16)
        return carry

    lax.fori_loop(0, mixes, last_body, 0)

    def sent(c, carry):
        own_part(c).wait_send()
        for k in range(1, n_chips):
            own_cross(c, k).wait_send()
            arrival(c, across(k), n_chips - 1 + k).wait_send()
        return carry

    def sent_mix(c, carry):
        for k in range(1, n_chips):
            cross_copy(k, c).wait_send()
        for k in range(n_chips):
            part_copy(k, c).wait_send()
        return carry

    lax.fori_loop(0, chunks, sent, 0)
    lax.fori_loop(0, mixes, sent_mix, 0)
    for k in range(1, n_sp):
        log_copy(k).wait_send()

    def sent_total(d, carry):
        total_arrival(d).wait_send()
        return carry

    lax.fori_loop(sp + 1, n_sp, sent_total, 0)
    lax.fori_loop(0, sp, sent_total, 0)


def body(n_sp, n_tp, tokens, norm_gain, w_q, w_k, w_v, w_rq, w_rk, w_rv, w_rg, att_sink,
         decay_log, init_state, out_att, out_ret):
    rows, chan = tokens.shape
    width = n_tp * chan
    ret = decay_log.shape[0]
    heads = att_sink.shape[0]
    kv_cols = w_k.shape[1]
    kv = kv_cols // HD
    chunks = rows // CHUNK
    n_chips = n_tp // 2
    weights = (w_q, w_k, w_v, w_rq, w_rk, w_rv, w_rg)
    names = ("q", "k", "v", "rq", "rk", "rv", "g")
    cols = [w.shape[1] for w in weights]
    joined = all(count % 128 == 0 for count in cols)
    places, dots = [], []
    if joined:
        buffers = [sum(cols)]
        at = 0
        for count in cols:
            places.append((0, at, count))
            at += count
        for group in ((0,), (1, 2), (3, 4), (5,), (6,)):
            dots.append((0, places[group[0]][1], sum(cols[i] for i in group),
                         tuple((names[i], cols[i]) for i in group)))
    else:
        buffers = cols
        for i, count in enumerate(cols):
            places.append((i, 0, count))
            dots.append((i, 0, count, ((names[i], count),)))
    cfg = dict(n_sp=n_sp, n_tp=n_tp, n_chips=n_chips, chunks=chunks, chan=chan, heads=heads,
               ret=ret, kv=kv, buffers=buffers, places=places, dots=dots, joined=joined)
    outer = rope_tables(n_sp * chunks, CHUNK, ret)
    inner = rope_tables(CHUNK, 1, ret)
    vmem = pl.BlockSpec(memory_space=pltpu.VMEM)
    anyw = pl.BlockSpec(memory_space=pl.ANY)
    smem = pl.BlockSpec(memory_space=pltpu.SMEM)
    dma = pltpu.SemaphoreType.DMA
    mixed_rows = heads * HD + ret * RV
    others = max(n_chips - 1, 1)
    scratch = [pltpu.VMEM((width, count), BF16) for count in buffers] + [
        pltpu.VMEM((n_tp, mixed_rows, chan), BF16),
        pltpu.VMEM((n_tp, rows, chan), BF16),
        pltpu.VMEM((CHUNK, width), BF16),
        pltpu.VMEM((rows, heads * HD), BF16),
        pltpu.VMEM((rows + 2 * WINDOW, kv_cols), BF16),
        pltpu.VMEM((rows + 2 * WINDOW, kv_cols), BF16),
        pltpu.VMEM((rows, heads * HD), BF16),
        pltpu.VMEM((ret, rows, 2 * RK), BF16),
        pltpu.VMEM((ret, rows, RV), F32),
        pltpu.VMEM((rows, ret * RV), BF16),
        pltpu.VMEM((ret, chunks, RK, RV), F32),
        pltpu.VMEM((ret, chunks, RK, RV), F32),
        pltpu.VMEM((ret, chunks, 8, 128), F32),
        pltpu.VMEM((ret, RK, RV), BF16),
        pltpu.VMEM((ret, RK, RV), BF16),
        pltpu.VMEM((n_sp, ret, RK, RV), BF16),
        pltpu.VMEM((n_sp, ret, 8, 128), F32),
        pltpu.VMEM((2, ret, RK, RV), F32),
        pltpu.VMEM((n_chips, rows, chan), F32),
        pltpu.VMEM((n_chips, rows, chan), BF16),
        pltpu.VMEM((n_chips, rows, chan), BF16),
        pltpu.VMEM((others, rows, chan), BF16),
        pltpu.VMEM((others, rows, chan), BF16),
        dma((7,)), dma((n_tp, 2)), dma,
        dma((2 * n_chips, chunks)), dma((n_tp, chunks)),
        dma((2, 2)), dma((2, 2)),
        dma((n_sp,)), dma((n_sp,)),
        dma((n_sp,)), dma((n_sp,)),
        dma((n_chips, rows // MIX)), dma((n_chips, rows // MIX)),
        dma((others, rows // MIX)), dma((others, rows // MIX)),
    ]
    return pl.pallas_call(
        functools.partial(kernel, cfg),
        out_shape=jax.ShapeDtypeStruct((rows, chan), BF16),
        in_specs=[anyw, vmem] + [anyw] * 7 + [smem, vmem, vmem, anyw, anyw] + [vmem] * 4,
        out_specs=vmem,
        scratch_shapes=scratch,
        compiler_params=pltpu.CompilerParams(
            collective_id=0, has_side_effects=True, vmem_limit_bytes=60 * 1024 * 1024),
    )(tokens, norm_gain.reshape(1, width), *weights, att_sink, decay_log, init_state,
      out_att, out_ret, *(jnp.asarray(t) for t in outer), *(jnp.asarray(t) for t in inner))


def solution(mesh):
    n_sp, n_tp = mesh.shape["sp"], mesh.shape["tp"]
    in_specs = (
        P("sp", "tp"),
        P(),
        P(None, "tp"),
        P(None, "tp"),
        P(None, "tp"),
        P(None, "tp"),
        P(None, "tp"),
        P(None, "tp"),
        P(None, "tp"),
        P("tp"),
        P("tp", "sp"),
        P(None, "tp", None, None),
        P("tp", None),
        P("tp", None),
    )
    return jax.shard_map(functools.partial(body, n_sp, n_tp), mesh=mesh, in_specs=in_specs,
                         out_specs=P("sp", "tp"), check_vma=False)
```
